32 devices in a mesh: rep: 2 (over x), fs: 4 (over z), tp: 4 (over y, core).
Axes of the slice: x: 2, y: 2, z: 4, core: 2. Of those that a mesh axis runs over, the one named last changes fastest.
Arguments:
- tokens: bfloat16 [4096, 2048], P(('rep', 'fs', 'tp')), may hold values from -6 to 6
- mixer_gain: float32 [2048], replicated, may hold values from 0.1 to 1.9
- direct_weight: float32 [2048, 1024], P('fs', 'tp'), may hold values from -0.125 to 0.125
- direct_scale: float32 [1024], P('tp'), may hold values from 0.5 to 2
- value_weight: float32 [2048, 1024], P('fs', 'tp'), may hold values from -0.125 to 0.125
- value_scale: float32 [1024], P('tp'), may hold values from 0.5 to 8, as said below
- value_gain: float32 [1024], P('tp'), may hold values from 0.1 to 1.9
- value_shift: float32 [1024], P('tp'), may hold values from -3 to 3
- spatial_weight: bfloat16 [16, 128, 128], P('tp'), may hold values from -0.25 to 0.25
- spatial_bias: float32 [16, 128], P('tp'), may hold values from 0.1 to 1.9
- merge_weight: float32 [1024, 2048], P('tp', 'fs'), may hold values from -0.1875 to 0.1875
- merge_scale: float32 [2048], P('fs'), may hold values from 0.5 to 2
- channel_gain: float32 [2048], replicated, may hold values from 0.1 to 1.9
- expand_weight: float32 [2048, 8192], P('fs', 'tp'), may hold values from -0.125 to 0.125
- expand_scale: float32 [8192], P('tp'), may hold values from 0.5 to 2
- reduce_weight: float32 [8192, 2048], P('tp', 'fs'), may hold values from -0.0625 to 0.0625
- reduce_scale: float32 [2048], P('fs'), may hold values from 0.5 to 2
Outputs:
- result: bfloat16 [4096, 2048], P(('rep', 'fs', 'tp'))
The draws below stay inside these ranges and needn't reach their ends.
Inputs may be any that keep to these rules, and one draw needn't show every extreme that they name: `value_scale`: positive column scales.
All inputs are finite; a program needn't handle non-finite values.
Results may differ from the reference program's by a relative error of at most 0.024.
Values may be sent and summed in bfloat16 or wider, within the bound.
A program may use at most 64 MiB of HBM per device.

```python
import math
import jax
import jax.numpy as jnp
from jax import lax

D = 2048
GROUPS = 16
GDIM = 64
AW = 1024
FF = 8192
BLOCK = 128
TOK_DEV = 128
TOKENS = 4096
N_TP = 4


def draw_value_scale(key, part):
    ramp = jnp.exp(jnp.log(4.0) * jnp.arange(AW, dtype=jnp.float32) / (AW - 1))
    factor = jnp.exp(jax.random.uniform(key, (AW,), jnp.float32, jnp.log(0.7), jnp.log(1.4)))
    return ramp * factor


def levels(stream_key, shape, shards, low, top_value):
    level = 1.0
    for axis_at, blocks in shards:
        draws = jax.random.uniform(jax.random.fold_in(jax.random.fold_in(stream_key, 6), axis_at), (blocks,), jnp.float32, low / len(shards), top_value / len(shards))
        level = level * jnp.repeat(jnp.exp(draws), shape[axis_at] // blocks).reshape((-1,) + (1,) * (len(shape) - 1 - axis_at))
    return level


def scatter_about(rng, extent, deviation, bound, shards=(), kind=jnp.bfloat16):
    result = jax.random.normal(rng, extent, jnp.float32) * deviation
    if len(shards) > 0:
        result = levels(rng, extent, shards, -0.22, 0.18) * result
    return jnp.clip(result, min=-bound, max=bound).astype(kind)


def setup_inputs(seed: int = 0) -> dict:
    seeds = jax.random.split(jax.random.key(seed), 18)
    tokens = scatter_about(seeds[0], (TOKENS, D), 1.0, 6.0, ((0, 32),))
    mixer_gain = jnp.clip(1.0 + 0.18 * jax.random.normal(seeds[1], (D,), jnp.float32), 0.1, 1.9)
    direct_weight = scatter_about(seeds[2], (D, AW), D ** -0.5, 0.125, ((0, 4), (1, 4)), jnp.float32)
    direct_scale = jnp.clip(jnp.exp(math.log(2.0) - 1.3862944 * jax.random.uniform(seeds[3], (AW,), jnp.float32) ** levels(seeds[3], (AW,), ((0, 4),), -0.2, 0.2)), 0.5, 2.0)
    value_weight = scatter_about(seeds[4], (D, AW), D ** -0.5, 0.125, ((0, 4), (1, 4)), jnp.float32)
    value_scale = draw_value_scale(jax.random.fold_in(seeds[17], 71), 0)
    value_gain = jnp.clip(1.0 + 0.18 * jax.random.normal(seeds[6], (AW,), jnp.float32), 0.1, 1.9)
    value_shift = scatter_about(seeds[7], (AW,), 0.5, 3.0, ((0, 4),), jnp.float32)
    spatial_weight = scatter_about(seeds[8], (GROUPS, BLOCK, BLOCK), (4 * BLOCK) ** -0.5, 0.25, ((0, 4),))
    spatial_bias = jnp.clip(1.0 + 0.18 * jax.random.normal(seeds[9], (GROUPS, BLOCK), jnp.float32), 0.1, 1.9)
    merge_weight = scatter_about(seeds[10], (AW, D), AW ** -0.5, 0.1875, ((0, 4), (1, 4)), jnp.float32)
    merge_scale = jnp.clip(jnp.exp(math.log(2.0) - 1.3862944 * jax.random.uniform(seeds[11], (D,), jnp.float32) ** levels(seeds[11], (D,), ((0, 4),), -0.2, 0.2)), 0.5, 2.0)
    channel_gain = jnp.clip(1.0 + 0.18 * jax.random.normal(seeds[12], (D,), jnp.float32), 0.1, 1.9)
    expand_weight = scatter_about(seeds[13], (D, FF), D ** -0.5, 0.125, ((0, 4), (1, 4)), jnp.float32)
    expand_scale = jnp.clip(jnp.exp(math.log(2.0) - 1.3862944 * jax.random.uniform(seeds[14], (FF,), jnp.float32) ** levels(seeds[14], (FF,), ((0, 4),), -0.2, 0.2)), 0.5, 2.0)
    reduce_weight = scatter_about(seeds[15], (FF, D), FF ** -0.5, 0.0625, ((0, 4), (1, 4)), jnp.float32)
    reduce_scale = jnp.clip(jnp.exp(math.log(2.0) - 1.3862944 * jax.random.uniform(seeds[16], (D,), jnp.float32) ** levels(seeds[16], (D,), ((0, 4),), -0.2, 0.2)), 0.5, 2.0)
    return {"tokens": tokens, "mixer_gain": mixer_gain, "direct_weight": direct_weight, "direct_scale": direct_scale, "value_weight": value_weight, "value_scale": value_scale, "value_gain": value_gain, "value_shift": value_shift, "spatial_weight": spatial_weight, "spatial_bias": spatial_bias, "merge_weight": merge_weight, "merge_scale": merge_scale, "channel_gain": channel_gain, "expand_weight": expand_weight, "expand_scale": expand_scale, "reduce_weight": reduce_weight, "reduce_scale": reduce_scale}


epsilon = 1e-06

def rms_rows(rows, gain):
    floats = rows.astype(jnp.float32)
    scaled = floats * lax.rsqrt(lax.optimization_barrier(jnp.mean(floats * floats, axis=-1, keepdims=True)) + epsilon)
    return (scaled * gain).astype(jnp.bfloat16)

def split_sum(left, right, scale, parts):
    rows = left.shape[0]
    inner = left.shape[1] // parts
    lhs = left.reshape(rows, parts, inner).astype(jnp.float32)
    rhs = right.astype(jnp.bfloat16).astype(jnp.float32).reshape(parts, inner, right.shape[1])
    terms = jnp.einsum('gtk,tkd->tgd', lhs, rhs) * scale
    terms = lax.optimization_barrier(terms.astype(jnp.bfloat16)).astype(jnp.float32)
    return lax.optimization_barrier(jnp.sum(terms, axis=0))

def reference(tokens, mixer_gain, direct_weight, direct_scale, value_weight, value_scale, value_gain, value_shift, spatial_weight, spatial_bias, merge_weight, merge_scale, channel_gain, expand_weight, expand_scale, reduce_weight, reduce_scale):
    seq_rows = TOK_DEV * N_TP

    def one_sequence(rows):
        normed = rms_rows(rows, mixer_gain)
        direct = jax.nn.gelu(jnp.dot(normed, direct_weight.astype(jnp.bfloat16), preferred_element_type=jnp.float32) * direct_scale)
        value = jax.nn.gelu(jnp.dot(normed, value_weight.astype(jnp.bfloat16), preferred_element_type=jnp.float32) * value_scale)
        total = lax.optimization_barrier(jnp.sum(value, axis=1, keepdims=True))
        squares = lax.optimization_barrier(jnp.sum(value * value, axis=1, keepdims=True))
        mean = total / AW
        var = squares / AW - mean * mean
        gated_value = ((value - mean) * lax.rsqrt(var + epsilon) * value_gain + value_shift).astype(jnp.bfloat16)
        blocks = gated_value.reshape(seq_rows // BLOCK, BLOCK, GROUPS, GDIM).astype(jnp.float32)
        mixed = jnp.einsum('gpq,nqgc->npgc', spatial_weight.astype(jnp.float32), blocks)
        mixed = mixed + jnp.transpose(spatial_bias)[None, :, :, None]
        gated = (direct * mixed.reshape(seq_rows, AW)).astype(jnp.bfloat16)
        mix = split_sum(gated, merge_weight, merge_scale, N_TP)
        middle = (rows.astype(jnp.float32) + mix).astype(jnp.bfloat16)
        normed_mid = rms_rows(middle, channel_gain)
        upper = jnp.dot(normed_mid, expand_weight.astype(jnp.bfloat16), preferred_element_type=jnp.float32) * expand_scale
        hidden = jnp.square(jax.nn.relu(upper)).astype(jnp.bfloat16)
        lower = split_sum(hidden, reduce_weight, reduce_scale, N_TP)
        return (middle.astype(jnp.float32) + lower).astype(jnp.bfloat16)
    grouped = tokens.reshape(-1, seq_rows, D)
    return lax.map(one_sequence, grouped).reshape(tokens.shape)
```

```python
import jax
import jax.numpy as jnp
from jax import lax
from jax.experimental import pallas as pl
from jax.experimental.pallas import tpu as pltpu
from jax.sharding import PartitionSpec as P

GDIM = 64
BLOCK = 128


epsilon = 1e-06


def rms_rows(rows, gain):
    floats = rows.astype(jnp.float32)
    scaled = floats * lax.rsqrt(jnp.mean(floats * floats, axis=-1, keepdims=True) + epsilon)
    return (scaled * gain).astype(jnp.bfloat16)


def body(
    tokens,
    mixer_gain,
    direct_weight,
    direct_scale,
    value_weight,
    value_scale,
    value_gain,
    value_shift,
    spatial_weight,
    spatial_bias,
    merge_weight,
    merge_scale,
    channel_gain,
    expand_weight,
    expand_scale,
    reduce_weight,
    reduce_scale,
):
    direct_half = direct_weight.astype(jnp.bfloat16)
    value_half = value_weight.astype(jnp.bfloat16)
    merge_half = merge_weight.astype(jnp.bfloat16)
    expand_half = expand_weight.astype(jnp.bfloat16)
    reduce_half = reduce_weight.astype(jnp.bfloat16)
    full_expand, full_reduce, reduce_full_scale = (
        lax.all_gather(expand_half, "fs", axis=0, tiled=True),
        lax.all_gather(reduce_half, "fs", axis=1, tiled=True),
        lax.all_gather(reduce_scale.astype(jnp.bfloat16), "fs", axis=0, tiled=True).astype(
            reduce_scale.dtype
        ),
    )
    normed = rms_rows(tokens, mixer_gain)
    whole = lax.all_gather(normed, "tp", axis=0, tiled=True)
    seq_rows = whole.shape[0]
    local_width = direct_weight.shape[1]
    direct_pre = jnp.dot(
        whole,
        lax.all_gather(direct_half, "fs", axis=0, tiled=True),
        preferred_element_type=jnp.float32,
    )
    value_pre = jnp.dot(
        whole,
        lax.all_gather(value_half, "fs", axis=0, tiled=True),
        preferred_element_type=jnp.float32,
    )
    full_merge, merge_full_scale = (
        lax.all_gather(merge_half, "fs", axis=1, tiled=True),
        lax.all_gather(merge_scale.astype(jnp.bfloat16), "fs", axis=0, tiled=True).astype(
            merge_scale.dtype
        ),
    )
    direct = jax.nn.gelu(direct_pre * direct_scale)
    value = jax.nn.gelu(value_pre * value_scale)
    total, squares = lax.psum((jnp.sum(value, axis=1), jnp.sum(value * value, axis=1)), "tp")
    branch_width = local_width * lax.axis_size("tp")
    mean = (total / branch_width)[:, None]
    var = (squares / branch_width)[:, None] - mean * mean
    gated_value = ((value - mean) * lax.rsqrt(var + epsilon) * value_gain + value_shift).astype(
        jnp.bfloat16
    )
    local_groups = spatial_weight.shape[0]
    blocks = gated_value.reshape(seq_rows // BLOCK, BLOCK, local_groups, GDIM)
    mixed = jnp.einsum("gpq,nqgc->npgc", spatial_weight, blocks, preferred_element_type=jnp.float32)
    mixed = mixed + jnp.transpose(spatial_bias)[None, :, :, None]
    gated = (direct * mixed.reshape(seq_rows, local_width)).astype(jnp.bfloat16)
    rows = gated
    mix = lax.psum_scatter(
        (jnp.dot(rows, full_merge, preferred_element_type=jnp.float32) * merge_full_scale).astype(
            jnp.bfloat16
        ),
        "tp",
        scatter_dimension=0,
        tiled=True,
    ).astype(jnp.float32)
    middle = (tokens.astype(jnp.float32) + mix).astype(jnp.bfloat16)
    normed_mid = rms_rows(middle, channel_gain)
    whole_mid = lax.all_gather(normed_mid, "tp", axis=0, tiled=True)
    upper = jnp.dot(whole_mid, full_expand, preferred_element_type=jnp.float32)
    hidden = jnp.square(jax.nn.relu(upper * expand_scale)).astype(jnp.bfloat16)
    rows = hidden
    lower = lax.psum_scatter(
        (jnp.dot(rows, full_reduce, preferred_element_type=jnp.float32) * reduce_full_scale).astype(
            jnp.bfloat16
        ),
        "tp",
        scatter_dimension=0,
        tiled=True,
    ).astype(jnp.float32)
    return (middle.astype(jnp.float32) + lower).astype(jnp.bfloat16)


MESH = pl.DeviceIdType.MESH


def fused_kernel(
    tok_ref, mgain_ref, dv_ref, dvscale_ref, vgain_ref, vshift_ref, sw_ref, sbias_ref,
    mg_ref, cgain_ref, ex_ref, exscale_ref, rd_ref,
    out_ref,
    dv_all, mg_all, ex_all, rd_all,
    xg, act, stat, gated, p1, r1, s1, x1, mid,
    nm, acc, hid, p2, r2, s2, x2,
    own_sem, wsend, wrecv, gsend, grecv, tsend, trecv, msend, mrecv, nsend, nrecv, fsend, frecv,
):
    rows, width = tok_ref.shape
    piece = dv_ref.shape[0]
    local = vgain_ref.shape[1]
    seq = xg.shape[0]
    r = lax.axis_index("rep")
    f = lax.axis_index("fs")
    t = lax.axis_index("tp")
    y, c = t // 2, t % 2
    right, left, across = (f + 1) % 4, (f + 3) % 4, (f + 2) % 4
    sib = {"tp": y * 2 + (1 - c)}
    ynb = {"tp": (1 - y) * 2 + c}
    xnb = {"rep": 1 - r}

    barrier = pltpu.get_barrier_semaphore()
    for dev in (sib, ynb, xnb, {"fs": right}, {"fs": left}):
        pl.semaphore_signal(barrier, inc=1, device_id=dev, device_id_type=MESH)
    pl.semaphore_wait(barrier, 5)

    def rcopy(src, dst, ssem, rsem, dev):
        return pltpu.make_async_remote_copy(
            src_ref=src, dst_ref=dst, send_sem=ssem, recv_sem=rsem,
            device_id=dev, device_id_type=MESH,
        )

    items = ((dv_ref, dv_all), (mg_ref, mg_all), (ex_ref, ex_all), (rd_ref, rd_all))

    def first(i, d):
        src, dst = items[i]
        return rcopy(
            src, dst.at[f], wsend.at[i, d, 0], wrecv.at[i, d, 0],
            {"fs": right if d == 0 else left},
        )

    def relay(i, d):
        dst = items[i][1]
        half = dst.shape[1] // 2
        part = dst.at[left if d == 0 else right, pl.ds(d * half, half)]
        return rcopy(
            part, part, wsend.at[i, d, 1], wrecv.at[i, d, 1],
            {"fs": right if d == 0 else left},
        )

    def first_start(i):
        for d in range(2):
            first(i, d).start()

    def relay_start(i):
        for d in range(2):
            first(i, d).wait_recv()
            relay(i, d).start()

    def relay_wait(i):
        for d in range(2):
            relay(i, d).wait_recv()

    first_start(0)
    first_start(1)
    owns = [
        pltpu.make_async_copy(src, dst.at[f], own_sem.at[i])
        for i, (src, dst) in enumerate(items)
    ]
    for own in owns:
        own.start()

    def norm(x, gain):
        return (
            x * lax.rsqrt(jnp.mean(x * x, axis=-1, keepdims=True) + epsilon) * gain
        ).astype(jnp.bfloat16)

    def block(n, size=1):
        return pl.ds(pl.multiple_of(n * rows, rows), size * rows)

    def columns(slot):
        return pl.ds(pl.multiple_of(slot * piece, piece), piece)

    mine = xg.at[block(c * 2 + y)]
    mine[...] = norm(tok_ref[...].astype(jnp.float32), mgain_ref[...])
    far = xg.at[block(c * 2 + 1 - y)]
    gather = (
        rcopy(mine, mine, gsend.at[0], grecv.at[0], sib),
        rcopy(mine, mine, gsend.at[1], grecv.at[1], ynb),
        rcopy(far, far, gsend.at[2], grecv.at[2], sib),
    )
    gather[1].start()
    gather[0].start()
    gather[1].wait_recv()
    gather[2].start()
    relay_start(0)
    relay_start(1)
    first_start(2)
    first_start(3)
    gather[0].wait_recv()
    gather[2].wait_recv()
    for own in owns:
        own.wait()

    def project(slot):
        return jnp.dot(xg[:, columns(slot)], dv_all[slot], preferred_element_type=jnp.float32)

    act[...] = project(f)
    act[...] += project(left)
    act[...] += project(right)
    relay_wait(0)
    act[...] = jax.nn.gelu((act[...] + project(across)) * dvscale_ref[...])

    lane = lax.broadcasted_iota(jnp.int32, (rows, rows), 1)
    for n in range(4):
        value = act[n * rows : (n + 1) * rows, local:]
        total = jnp.sum(value, axis=1, keepdims=True)
        squares = jnp.sum(value * value, axis=1, keepdims=True)
        table = jnp.where(lane == 0, total, jnp.where(lane == 1, squares, 0.0))
        stat[t, n] = jnp.transpose(table)[:8]
    stats = [
        rcopy(stat.at[t], stat.at[t], tsend.at[0], trecv.at[0], sib),
        rcopy(stat.at[t], stat.at[t], tsend.at[1], trecv.at[1], ynb),
        rcopy(
            stat.at[(1 - y) * 2 + c], stat.at[(1 - y) * 2 + c], tsend.at[2], trecv.at[2], sib
        ),
    ]
    stats[1].start()
    stats[0].start()
    stats[1].wait_recv()
    stats[2].start()
    stats[0].wait_recv()
    stats[2].wait_recv()
    inverse = 1.0 / (local * 4)
    group_lane = lax.broadcasted_iota(jnp.int32, (rows, 128), 1) // GDIM
    for n in range(4):
        here = slice(n * rows, (n + 1) * rows)
        summed = stat[0, n] + stat[1, n] + stat[2, n] + stat[3, n]
        table = jnp.transpose(jnp.concatenate([summed] * (rows // 8), axis=0))
        mean = table[:, 0:1] * inverse
        var = table[:, 1:2] * inverse - mean * mean
        gv = (
            (act[here, local:] - mean) * lax.rsqrt(var + epsilon) * vgain_ref[...]
            + vshift_ref[...]
        ).astype(jnp.bfloat16)
        per = 128 // GDIM
        for j in range(local // 128):
            at = slice(j * 128, (j + 1) * 128)
            mixed = jnp.dot(sw_ref[j * per], gv[:, at], preferred_element_type=jnp.float32)
            for k in range(1, per):
                other = jnp.dot(
                    sw_ref[j * per + k], gv[:, at], preferred_element_type=jnp.float32
                )
                mixed = jnp.where(group_lane == k, other, mixed)
            gated[here, at] = (act[here, at] * (mixed + sbias_ref[:, at])).astype(jnp.bfloat16)

    slots = (f, left, right, across)

    def merge_pair(k):
        return rcopy(
            p1.at[k, block((1 - c) * 2, 2)], r1.at[k], msend.at[k, 0], mrecv.at[k, 0], sib
        )

    def merge_far(k):
        return rcopy(s1.at[k], x1.at[k], msend.at[k, 1], mrecv.at[k, 1], ynb)

    def merge_send(k):
        merge_pair(k).wait_recv()
        s1[k] = (
            p1[k, block(c * 2 + 1 - y)].astype(jnp.float32)
            + r1[k, block(1 - y)].astype(jnp.float32)
        ).astype(jnp.bfloat16)
        merge_far(k).start()

    for k, slot in enumerate(slots):
        if k == 3:
            relay_wait(1)
        p1[k] = jnp.dot(gated[...], mg_all[slot], preferred_element_type=jnp.float32).astype(
            jnp.bfloat16
        )
        merge_pair(k).start()
        if k > 0:
            merge_send(k - 1)
    merge_send(3)
    for k, slot in enumerate(slots):
        merge_far(k).wait_recv()
        mid[:, columns(slot)] = (
            tok_ref[:, columns(slot)].astype(jnp.float32)
            + p1[k, block(c * 2 + y)].astype(jnp.float32)
            + r1[k, block(y)].astype(jnp.float32)
            + x1[k].astype(jnp.float32)
        ).astype(jnp.bfloat16)

    def place(rr, yy):
        return nm.at[block(c * 4 + rr * 2 + yy)]

    half = rows // 2
    mine = place(r, y)
    mine[...] = norm(mid[...].astype(jnp.float32), cgain_ref[...])
    from_x, from_y, from_xy = place(1 - r, y), place(r, 1 - y), place(1 - r, 1 - y)
    low, high = from_x.at[pl.ds(0, half)], from_y.at[pl.ds(half, half)]
    spread = (
        rcopy(mine, mine, nsend.at[0], nrecv.at[0], xnb),
        rcopy(mine, mine, nsend.at[1], nrecv.at[1], ynb),
        rcopy(mine, mine, nsend.at[2], nrecv.at[2], sib),
        rcopy(low, low, nsend.at[3], nrecv.at[3], ynb),
        rcopy(high, high, nsend.at[4], nrecv.at[4], xnb),
        rcopy(from_x, from_x, nsend.at[5], nrecv.at[5], sib),
        rcopy(from_y, from_y, nsend.at[6], nrecv.at[6], sib),
        rcopy(from_xy, from_xy, nsend.at[7], nrecv.at[7], sib),
    )
    for k in range(3):
        spread[k].start()
    relay_start(2)
    spread[0].wait_recv()
    spread[3].start()
    spread[5].start()
    spread[1].wait_recv()
    spread[4].start()
    spread[6].start()
    relay_start(3)
    spread[3].wait_recv()
    spread[4].wait_recv()
    spread[7].start()
    for k in (2, 5, 6, 7):
        spread[k].wait_recv()

    everyone = nm.shape[0]
    tall = 2 * rows

    def over_rows(step):
        lax.fori_loop(
            0, everyone // tall,
            lambda i, _: step(pl.ds(pl.multiple_of(i * tall, tall), tall)), None,
        )

    def expand(at, slot):
        return jnp.dot(nm[at, columns(slot)], ex_all[slot], preferred_element_type=jnp.float32)

    def expand_most(at):
        acc[at] = expand(at, f) + expand(at, left) + expand(at, right)

    def expand_last(at):
        upper = (acc[at] + expand(at, across)) * exscale_ref[...]
        hid[at] = jnp.square(jax.nn.relu(upper)).astype(jnp.bfloat16)

    over_rows(expand_most)
    relay_wait(2)
    over_rows(expand_last)

    def down_pair(k):
        return rcopy(
            p2.at[k, block((1 - c) * 4, 4)], r2.at[k], fsend.at[k, 0], frecv.at[k, 0], sib
        )

    hops = ((1 - r, y), (r, 1 - y), (1 - r, 1 - y))

    def down_far(k, h):
        rr, yy = hops[h]
        dev = (xnb, ynb)[h]
        return rcopy(
            s2.at[k, block(rr * 2 + yy)], x2.at[k, h], fsend.at[k, 1 + h], frecv.at[k, 1 + h], dev
        )

    def down_via(k, h):
        return rcopy(
            s2.at[k, pl.ds(pl.multiple_of((hops[2][0] * 2 + hops[2][1]) * rows + h * half, half), half)],
            x2.at[k, 2, pl.ds(h * half, half)],
            fsend.at[k, 3 + h], frecv.at[k, 3 + h], (xnb, ynb)[h],
        )

    def down_on(k, h):
        return rcopy(
            x2.at[k, 2, pl.ds(h * half, half)], x2.at[k, 3, pl.ds(h * half, half)],
            fsend.at[k, 5 + h], frecv.at[k, 5 + h], (ynb, xnb)[h],
        )

    def down_send(k):
        down_pair(k).wait_recv()
        s2[k] = (
            p2[k, block(c * 4, 4)].astype(jnp.float32) + r2[k].astype(jnp.float32)
        ).astype(jnp.bfloat16)
        for h in range(2):
            down_via(k, h).start()
        for h in range(2):
            down_far(k, h).start()

    def down_relay(k):
        for h in range(2):
            down_via(k, h).wait_recv()
            down_on(k, h).start()

    for k, slot in enumerate(slots):
        if k == 3:
            relay_wait(3)

        def reduce(at, k=k, slot=slot):
            p2[k, at] = jnp.dot(
                hid[at], rd_all[slot], preferred_element_type=jnp.float32
            ).astype(jnp.bfloat16)

        over_rows(reduce)
        down_pair(k).start()
        if k > 0:
            down_send(k - 1)
        if k > 1:
            down_relay(k - 2)
    down_send(3)
    down_relay(2)
    down_relay(3)
    for k, slot in enumerate(slots):
        for h in range(2):
            down_far(k, h).wait_recv()
            down_on(k, h).wait_recv()
        out_ref[:, columns(slot)] = (
            mid[:, columns(slot)].astype(jnp.float32)
            + p2[k, block(c * 4 + r * 2 + y)].astype(jnp.float32)
            + r2[k, block(r * 2 + y)].astype(jnp.float32)
            + x2[k, 0].astype(jnp.float32)
            + x2[k, 1].astype(jnp.float32)
            + x2[k, 3].astype(jnp.float32)
        ).astype(jnp.bfloat16)

    for i in range(4):
        for d in range(2):
            first(i, d).wait_send()
            relay(i, d).wait_send()
    for copy in gather + tuple(stats) + spread:
        copy.wait_send()
    for k in range(4):
        merge_pair(k).wait_send()
        merge_far(k).wait_send()
        down_pair(k).wait_send()
        for h in range(2):
            down_far(k, h).wait_send()
            down_via(k, h).wait_send()
            down_on(k, h).wait_send()


def fused_body(
    tokens,
    mixer_gain,
    direct_weight,
    direct_scale,
    value_weight,
    value_scale,
    value_gain,
    value_shift,
    spatial_weight,
    spatial_bias,
    merge_weight,
    merge_scale,
    channel_gain,
    expand_weight,
    expand_scale,
    reduce_weight,
    reduce_scale,
):
    bf = jnp.bfloat16
    rows, width = tokens.shape
    piece, local = direct_weight.shape
    wide = expand_weight.shape[1] // 2
    r = lax.axis_index("rep")
    dv = jnp.concatenate([direct_weight.astype(bf), value_weight.astype(bf)], axis=1)
    dvscale = jnp.concatenate([direct_scale, value_scale])[None]
    sbias = jnp.repeat(jnp.transpose(spatial_bias), GDIM, axis=1)
    mg = (merge_weight * merge_scale).astype(bf)
    ex = lax.dynamic_slice_in_dim(expand_weight, r * wide, wide, 1).astype(bf)
    exscale = lax.dynamic_slice_in_dim(expand_scale, r * wide, wide, 0)[None]
    rd = (lax.dynamic_slice_in_dim(reduce_weight, r * wide, wide, 0) * reduce_scale).astype(bf)
    seq = 4 * rows
    vm = pltpu.VMEM
    dma = pltpu.SemaphoreType.DMA
    f32 = jnp.float32
    operands = (
        tokens, mixer_gain[None], dv, dvscale, value_gain[None], value_shift[None],
        spatial_weight, sbias, mg, channel_gain[None], ex, exscale, rd,
    )
    return pl.pallas_call(
        fused_kernel,
        out_shape=jax.ShapeDtypeStruct((rows, width), bf),
        in_specs=[pl.BlockSpec(memory_space=pltpu.VMEM)] * len(operands),
        out_specs=pl.BlockSpec(memory_space=pltpu.VMEM),
        scratch_shapes=[
            vm((4, piece, 2 * local), bf),
            vm((4, local, piece), bf),
            vm((4, piece, wide), bf),
            vm((4, wide, piece), bf),
            vm((seq, width), bf),
            vm((seq, 2 * local), f32),
            vm((4, 4, 8, rows), f32),
            vm((seq, local), bf),
            vm((4, seq, piece), bf),
            vm((4, 2 * rows, piece), bf),
            vm((4, rows, piece), bf),
            vm((4, rows, piece), bf),
            vm((rows, width), bf),
            vm((2 * seq, width), bf),
            vm((2 * seq, wide), f32),
            vm((2 * seq, wide), bf),
            vm((4, 2 * seq, piece), bf),
            vm((4, seq, piece), bf),
            vm((4, seq, piece), bf),
            vm((4, 4, rows, piece), bf),
            dma((4,)),
            dma((4, 2, 2)), dma((4, 2, 2)),
            dma((3,)), dma((3,)),
            dma((3,)), dma((3,)),
            dma((4, 2)), dma((4, 2)),
            dma((8,)), dma((8,)),
            dma((4, 7)), dma((4, 7)),
        ],
        compiler_params=pltpu.CompilerParams(
            collective_id=0, has_side_effects=True, vmem_limit_bytes=60 * 1024 * 1024
        ),
    )(*operands)


def solution(mesh):
    sizes = mesh.shape
    fused = sizes["rep"] == 2 and sizes["fs"] == 4 and sizes["tp"] == 4
    return jax.shard_map(
        fused_body if fused else body,
        mesh=mesh,
        in_specs=(
            P(("rep", "fs", "tp"), None),
            P(),
            P("fs", "tp"),
            P("tp"),
            P("fs", "tp"),
            P("tp"),
            P("tp"),
            P("tp"),
            P("tp", None, None),
            P("tp", None),
            P("tp", "fs"),
            P("fs"),
            P(),
            P("fs", "tp"),
            P("tp"),
            P("tp", "fs"),
            P("fs"),
        ),
        out_specs=P(("rep", "fs", "tp"), None),
        check_vma=False,
    )
```

```python
import jax
import jax.numpy as jnp
from jax import lax
from jax.experimental import pallas as pl
from jax.experimental.pallas import tpu as pltpu
from jax.sharding import PartitionSpec as P

GDIM = 64
BLOCK = 128


epsilon = 1e-06


def rms_rows(rows, gain):
    floats = rows.astype(jnp.float32)
    scaled = floats * lax.rsqrt(jnp.mean(floats * floats, axis=-1, keepdims=True) + epsilon)
    return (scaled * gain).astype(jnp.bfloat16)


def body(
    tokens,
    mixer_gain,
    direct_weight,
    direct_scale,
    value_weight,
    value_scale,
    value_gain,
    value_shift,
    spatial_weight,
    spatial_bias,
    merge_weight,
    merge_scale,
    channel_gain,
    expand_weight,
    expand_scale,
    reduce_weight,
    reduce_scale,
):
    direct_half = direct_weight.astype(jnp.bfloat16)
    value_half = value_weight.astype(jnp.bfloat16)
    merge_half = merge_weight.astype(jnp.bfloat16)
    expand_half = expand_weight.astype(jnp.bfloat16)
    reduce_half = reduce_weight.astype(jnp.bfloat16)
    full_expand, full_reduce, reduce_full_scale = (
        lax.all_gather(expand_half, "fs", axis=0, tiled=True),
        lax.all_gather(reduce_half, "fs", axis=1, tiled=True),
        lax.all_gather(reduce_scale.astype(jnp.bfloat16), "fs", axis=0, tiled=True).astype(
            reduce_scale.dtype
        ),
    )
    normed = rms_rows(tokens, mixer_gain)
    whole = lax.all_gather(normed, "tp", axis=0, tiled=True)
    seq_rows = whole.shape[0]
    local_width = direct_weight.shape[1]
    direct_pre = jnp.dot(
        whole,
        lax.all_gather(direct_half, "fs", axis=0, tiled=True),
        preferred_element_type=jnp.float32,
    )
    value_pre = jnp.dot(
        whole,
        lax.all_gather(value_half, "fs", axis=0, tiled=True),
        preferred_element_type=jnp.float32,
    )
    full_merge, merge_full_scale = (
        lax.all_gather(merge_half, "fs", axis=1, tiled=True),
        lax.all_gather(merge_scale.astype(jnp.bfloat16), "fs", axis=0, tiled=True).astype(
            merge_scale.dtype
        ),
    )
    direct = jax.nn.gelu(direct_pre * direct_scale)
    value = jax.nn.gelu(value_pre * value_scale)
    total, squares = lax.psum((jnp.sum(value, axis=1), jnp.sum(value * value, axis=1)), "tp")
    branch_width = local_width * lax.axis_size("tp")
    mean = (total / branch_width)[:, None]
    var = (squares / branch_width)[:, None] - mean * mean
    gated_value = ((value - mean) * lax.rsqrt(var + epsilon) * value_gain + value_shift).astype(
        jnp.bfloat16
    )
    local_groups = spatial_weight.shape[0]
    blocks = gated_value.reshape(seq_rows // BLOCK, BLOCK, local_groups, GDIM)
    mixed = jnp.einsum("gpq,nqgc->npgc", spatial_weight, blocks, preferred_element_type=jnp.float32)
    mixed = mixed + jnp.transpose(spatial_bias)[None, :, :, None]
    gated = (direct * mixed.reshape(seq_rows, local_width)).astype(jnp.bfloat16)
    rows = gated
    mix = lax.psum_scatter(
        (jnp.dot(rows, full_merge, preferred_element_type=jnp.float32) * merge_full_scale).astype(
            jnp.bfloat16
        ),
        "tp",
        scatter_dimension=0,
        tiled=True,
    ).astype(jnp.float32)
    middle = (tokens.astype(jnp.float32) + mix).astype(jnp.bfloat16)
    normed_mid = rms_rows(middle, channel_gain)
    whole_mid = lax.all_gather(normed_mid, "tp", axis=0, tiled=True)
    upper = jnp.dot(whole_mid, full_expand, preferred_element_type=jnp.float32)
    hidden = jnp.square(jax.nn.relu(upper * expand_scale)).astype(jnp.bfloat16)
    rows = hidden
    lower = lax.psum_scatter(
        (jnp.dot(rows, full_reduce, preferred_element_type=jnp.float32) * reduce_full_scale).astype(
            jnp.bfloat16
        ),
        "tp",
        scatter_dimension=0,
        tiled=True,
    ).astype(jnp.float32)
    return (middle.astype(jnp.float32) + lower).astype(jnp.bfloat16)


MESH = pl.DeviceIdType.MESH


def fused_kernel(
    tok_ref, mgain_ref, dv_ref, dvscale_ref, vgain_ref, vshift_ref, sw_ref, sbias_ref,
    mg_ref, cgain_ref, ex_ref, exscale_ref, rd_ref,
    out_ref,
    dv_all, mg_all, ex_all, rd_all,
    xg, act, stat, gated, p1, r1, s1, x1, mid,
    nm, acc, hid, p2, r2, s2, z2, s3, x2,
    own_sem, wsend, wrecv, xsend, xrecv, gsend, grecv, tsend, trecv, msend, mrecv, nsend, nrecv, fsend, frecv,
):
    rows, width = tok_ref.shape
    piece = dv_ref.shape[0]
    local = vgain_ref.shape[1]
    seq = xg.shape[0]
    r = lax.axis_index("rep")
    f = lax.axis_index("fs")
    t = lax.axis_index("tp")
    y, c = t // 2, t % 2
    z = f % 2
    mate = f + 1 - 2 * z
    peers = (mate, (f + 2) % 4, (mate + 2) % 4)
    sib = {"tp": y * 2 + (1 - c)}
    ynb = {"tp": (1 - y) * 2 + c}
    xnb = {"rep": 1 - r}
    znb = {"fs": mate}

    barrier = pltpu.get_barrier_semaphore()
    for dev in (sib, ynb, xnb) + tuple({"fs": peer} for peer in peers):
        pl.semaphore_signal(barrier, inc=1, device_id=dev, device_id_type=MESH)
    pl.semaphore_wait(barrier, 6)

    def rcopy(src, dst, ssem, rsem, dev):
        return pltpu.make_async_remote_copy(
            src_ref=src, dst_ref=dst, send_sem=ssem, recv_sem=rsem,
            device_id=dev, device_id_type=MESH,
        )

    mixer = ((dv_ref, dv_all), (mg_ref, mg_all))

    def part(i, slot, q):
        ref = mixer[i][1]
        size = ref.shape[1] // 2
        return ref.at[slot, pl.ds(pl.multiple_of(q * size, size), size)]

    def along(i, j):
        src = mixer[i][0]
        size = src.shape[0] // 2
        return rcopy(
            src.at[pl.ds(pl.multiple_of(r * size, size), size)], part(i, f, r),
            wsend.at[i, j], wrecv.at[i, j], {"fs": peers[j]},
        )

    def over(i, j):
        here = part(i, peers[j], r)
        return rcopy(here, here, xsend.at[i, j], xrecv.at[i, j], xnb)

    def over_start(i):
        for j in range(3):
            along(i, j).wait_recv()
            over(i, j).start()

    def over_wait(i):
        for j in range(3):
            over(i, j).wait_recv()

    def chunk(i, j):
        to = peers[j] % 2
        src = ex_ref.at[to] if i == 2 else rd_ref.at[to, i - 3]
        dst = ex_all.at[f] if i == 2 else rd_all.at[f, i - 3]
        return rcopy(src, dst, wsend.at[i, j], wrecv.at[i, j], {"fs": peers[j]})

    for i in range(2):
        for j in range(3):
            along(i, j).start()
    for i in range(2, 5):
        for j in range(3):
            chunk(i, j).start()
    owns = [
        pltpu.make_async_copy(src, dst.at[f], own_sem.at[i])
        for i, (src, dst) in enumerate(
            mixer + ((ex_ref.at[z], ex_all), (rd_ref.at[z], rd_all))
        )
    ]
    for own in owns:
        own.start()

    def norm(x, gain):
        return (
            x * lax.rsqrt(jnp.mean(x * x, axis=-1, keepdims=True) + epsilon) * gain
        ).astype(jnp.bfloat16)

    def block(n, size=1):
        return pl.ds(pl.multiple_of(n * rows, rows), size * rows)

    def columns(slot):
        return pl.ds(pl.multiple_of(slot * piece, piece), piece)

    mine = xg.at[block(c * 2 + y)]
    mine[...] = norm(tok_ref[...].astype(jnp.float32), mgain_ref[...])
    far = xg.at[block(c * 2 + 1 - y)]
    gather = (
        rcopy(mine, mine, gsend.at[0], grecv.at[0], sib),
        rcopy(mine, mine, gsend.at[1], grecv.at[1], ynb),
        rcopy(far, far, gsend.at[2], grecv.at[2], sib),
    )
    gather[1].start()
    gather[0].start()
    gather[1].wait_recv()
    gather[2].start()
    over_start(0)
    over_start(1)
    gather[0].wait_recv()
    gather[2].wait_recv()
    for own in owns:
        own.wait()

    def project(slot):
        return jnp.dot(xg[:, columns(slot)], dv_all[slot], preferred_element_type=jnp.float32)

    over_wait(0)
    act[...] = project(f)
    for peer in peers:
        act[...] += project(peer)
    act[...] = jax.nn.gelu(act[...] * dvscale_ref[...])

    lane = lax.broadcasted_iota(jnp.int32, (rows, rows), 1)
    for n in range(4):
        value = act[n * rows : (n + 1) * rows, local:]
        total = jnp.sum(value, axis=1, keepdims=True)
        squares = jnp.sum(value * value, axis=1, keepdims=True)
        table = jnp.where(lane == 0, total, jnp.where(lane == 1, squares, 0.0))
        stat[t, n] = jnp.transpose(table)[:8]
    stats = [
        rcopy(stat.at[t], stat.at[t], tsend.at[0], trecv.at[0], sib),
        rcopy(stat.at[t], stat.at[t], tsend.at[1], trecv.at[1], ynb),
        rcopy(
            stat.at[(1 - y) * 2 + c], stat.at[(1 - y) * 2 + c], tsend.at[2], trecv.at[2], sib
        ),
    ]
    stats[1].start()
    stats[0].start()
    stats[1].wait_recv()
    stats[2].start()
    stats[0].wait_recv()
    stats[2].wait_recv()
    inverse = 1.0 / (local * 4)
    group_lane = lax.broadcasted_iota(jnp.int32, (rows, 128), 1) // GDIM
    for n in range(4):
        here = slice(n * rows, (n + 1) * rows)
        summed = stat[0, n] + stat[1, n] + stat[2, n] + stat[3, n]
        table = jnp.transpose(jnp.concatenate([summed] * (rows // 8), axis=0))
        mean = table[:, 0:1] * inverse
        var = table[:, 1:2] * inverse - mean * mean
        gv = (
            (act[here, local:] - mean) * lax.rsqrt(var + epsilon) * vgain_ref[...]
            + vshift_ref[...]
        ).astype(jnp.bfloat16)
        per = 128 // GDIM
        for j in range(local // 128):
            at = slice(j * 128, (j + 1) * 128)
            mixed = jnp.dot(sw_ref[j * per], gv[:, at], preferred_element_type=jnp.float32)
            for k in range(1, per):
                other = jnp.dot(
                    sw_ref[j * per + k], gv[:, at], preferred_element_type=jnp.float32
                )
                mixed = jnp.where(group_lane == k, other, mixed)
            gated[here, at] = (act[here, at] * (mixed + sbias_ref[:, at])).astype(jnp.bfloat16)

    slots = (f,) + peers

    def merge_pair(k):
        return rcopy(
            p1.at[k, block((1 - c) * 2, 2)], r1.at[k], msend.at[k, 0], mrecv.at[k, 0], sib
        )

    def merge_far(k):
        return rcopy(s1.at[k], x1.at[k], msend.at[k, 1], mrecv.at[k, 1], ynb)

    def merge_send(k):
        merge_pair(k).wait_recv()
        s1[k] = (
            p1[k, block(c * 2 + 1 - y)].astype(jnp.float32)
            + r1[k, block(1 - y)].astype(jnp.float32)
        ).astype(jnp.bfloat16)
        merge_far(k).start()

    for k, slot in enumerate(slots):
        if k == 1:
            over_wait(1)
        p1[k] = jnp.dot(gated[...], mg_all[slot], preferred_element_type=jnp.float32).astype(
            jnp.bfloat16
        )
        merge_pair(k).start()
        if k > 0:
            merge_send(k - 1)
    merge_send(3)
    for k, slot in enumerate(slots):
        merge_far(k).wait_recv()
        mid[:, columns(slot)] = (
            tok_ref[:, columns(slot)].astype(jnp.float32)
            + p1[k, block(c * 2 + y)].astype(jnp.float32)
            + r1[k, block(y)].astype(jnp.float32)
            + x1[k].astype(jnp.float32)
        ).astype(jnp.bfloat16)

    def place(zz, rr, yy):
        return nm.at[block(c * 8 + zz * 4 + rr * 2 + yy)]

    half = rows // 2
    mine = place(z, r, y)
    mine[...] = norm(mid[...].astype(jnp.float32), cgain_ref[...])
    over_fs = rcopy(mine, mine, nsend.at[16], nrecv.at[16], znb)

    def spreading(b, zz):
        here = place(zz, r, y)
        from_x, from_y = place(zz, 1 - r, y), place(zz, r, 1 - y)
        from_xy = place(zz, 1 - r, 1 - y)
        low, high = from_x.at[pl.ds(0, half)], from_y.at[pl.ds(half, half)]
        routes = (
            (here, xnb), (here, ynb), (here, sib), (low, ynb), (high, xnb),
            (from_x, sib), (from_y, sib), (from_xy, sib),
        )
        return tuple(
            rcopy(ref, ref, nsend.at[8 * b + k], nrecv.at[8 * b + k], dev)
            for k, (ref, dev) in enumerate(routes)
        )

    near, far = spreading(0, z), spreading(1, 1 - z)
    over_fs.start()
    for k in range(3):
        near[k].start()
    over_fs.wait_recv()
    for k in range(3):
        far[k].start()
    for spread in (near, far):
        for k in range(2):
            spread[k].wait_recv()
            spread[3 + k].start()
            spread[5 + k].start()
    for spread in (near, far):
        spread[3].wait_recv()
        spread[4].wait_recv()
        spread[7].start()
    for spread in (near, far):
        for k in (2, 5, 6, 7):
            spread[k].wait_recv()

    everyone = nm.shape[0]
    tall = 2 * rows

    def over_rows(step):
        lax.fori_loop(
            0, everyone // tall,
            lambda i, _: step(pl.ds(pl.multiple_of(i * tall, tall), tall)), None,
        )

    def expand(at, slot):
        return jnp.dot(nm[at, columns(slot)], ex_all[slot], preferred_element_type=jnp.float32)

    def expand_most(at):
        acc[at] = expand(at, f) + expand(at, peers[0])

    def expand_last(at):
        upper = (acc[at] + expand(at, peers[1]) + expand(at, peers[2])) * exscale_ref[...]
        hid[at] = jnp.square(jax.nn.relu(upper)).astype(jnp.bfloat16)

    chunk(2, 0).wait_recv()
    over_rows(expand_most)
    chunk(2, 1).wait_recv()
    chunk(2, 2).wait_recv()
    over_rows(expand_last)

    def down_pair(k):
        return rcopy(
            p2.at[k, block((1 - c) * 8, 8)], r2.at[k], fsend.at[k, 0], frecv.at[k, 0], sib
        )

    def down_fs(k):
        return rcopy(
            s2.at[k], z2.at[k], fsend.at[k, 7], frecv.at[k, 7], znb
        )

    def down_fs_send(k):
        down_pair(k).wait_recv()
        s2[k] = (
            p2[k, block(c * 8 + (1 - z) * 4, 4)].astype(jnp.float32)
            + r2[k, block((1 - z) * 4, 4)].astype(jnp.float32)
        ).astype(jnp.bfloat16)
        down_fs(k).start()

    hops = ((1 - r, y), (r, 1 - y), (1 - r, 1 - y))

    def down_far(k, h):
        rr, yy = hops[h]
        dev = (xnb, ynb)[h]
        return rcopy(
            s3.at[k, block(rr * 2 + yy)], x2.at[k, h], fsend.at[k, 1 + h], frecv.at[k, 1 + h], dev
        )

    def down_via(k, h):
        return rcopy(
            s3.at[k, pl.ds(pl.multiple_of((hops[2][0] * 2 + hops[2][1]) * rows + h * half, half), half)],
            x2.at[k, 2, pl.ds(h * half, half)],
            fsend.at[k, 3 + h], frecv.at[k, 3 + h], (xnb, ynb)[h],
        )

    def down_on(k, h):
        return rcopy(
            x2.at[k, 2, pl.ds(h * half, half)], x2.at[k, 3, pl.ds(h * half, half)],
            fsend.at[k, 5 + h], frecv.at[k, 5 + h], (ynb, xnb)[h],
        )

    def down_send(k):
        down_fs(k).wait_recv()
        s3[k] = (
            p2[k, block(c * 8 + z * 4, 4)].astype(jnp.float32)
            + r2[k, block(z * 4, 4)].astype(jnp.float32)
            + z2[k].astype(jnp.float32)
        ).astype(jnp.bfloat16)
        for h in range(2):
            down_via(k, h).start()
        for h in range(2):
            down_far(k, h).start()

    def down_relay(k):
        for h in range(2):
            down_via(k, h).wait_recv()
            down_on(k, h).start()

    steps = ((0, 0), (1, 0), (0, 1), (1, 1), (2, 0), (3, 0), (2, 1), (3, 1))
    base = f - z
    order = (base, base + 1, 2 - base, 3 - base)

    def arrived(side, j):
        rcopy(
            rd_ref.at[0, side], rd_all.at[f, side],
            wsend.at[3 + side, j], wrecv.at[3 + side, j], znb,
        ).wait_recv()

    last = len(steps)
    thin = piece // 2

    for k in range(last + 3):
        if k < last:
            from_slot, side = steps[k]
            slot = order[from_slot]
            if from_slot == 0:
                arrived(side, 0)
            elif from_slot > 1:
                arrived(side, 1 + (from_slot + z) % 2)

            def reduce(at, k=k, slot=slot, side=side):
                p2[k, at] = jnp.dot(
                    hid[at], rd_all[slot, side], preferred_element_type=jnp.float32
                ).astype(jnp.bfloat16)

            over_rows(reduce)
            down_pair(k).start()
        if 0 < k <= last:
            down_fs_send(k - 1)
        if 1 < k <= last + 1:
            down_send(k - 2)
        if 2 < k:
            down_relay(k - 3)
    for k, (from_slot, side) in enumerate(steps):
        for h in range(2):
            down_far(k, h).wait_recv()
            down_on(k, h).wait_recv()
        at = pl.ds(pl.multiple_of(order[from_slot] * piece + side * thin, thin), thin)
        out_ref[:, at] = (
            mid[:, at].astype(jnp.float32)
            + p2[k, block(c * 8 + z * 4 + r * 2 + y)].astype(jnp.float32)
            + r2[k, block(z * 4 + r * 2 + y)].astype(jnp.float32)
            + z2[k, block(r * 2 + y)].astype(jnp.float32)
            + x2[k, 0].astype(jnp.float32)
            + x2[k, 1].astype(jnp.float32)
            + x2[k, 3].astype(jnp.float32)
        ).astype(jnp.bfloat16)

    for j in range(3):
        for i in range(2):
            along(i, j).wait_send()
            over(i, j).wait_send()
        for i in range(2, 5):
            chunk(i, j).wait_send()
    for copy in gather + tuple(stats) + near + far + (over_fs,):
        copy.wait_send()
    for k in range(4):
        merge_pair(k).wait_send()
        merge_far(k).wait_send()
    for k in range(last):
        down_pair(k).wait_send()
        down_fs(k).wait_send()
        for h in range(2):
            down_far(k, h).wait_send()
            down_via(k, h).wait_send()
            down_on(k, h).wait_send()


def fused_body(
    tokens,
    mixer_gain,
    direct_weight,
    direct_scale,
    value_weight,
    value_scale,
    value_gain,
    value_shift,
    spatial_weight,
    spatial_bias,
    merge_weight,
    merge_scale,
    channel_gain,
    expand_weight,
    expand_scale,
    reduce_weight,
    reduce_scale,
):
    bf = jnp.bfloat16
    rows, width = tokens.shape
    piece, local = direct_weight.shape
    wide = expand_weight.shape[1] // 2
    r = lax.axis_index("rep")
    unit = wide // 2
    f = lax.axis_index("fs")
    dv = jnp.concatenate([direct_weight.astype(bf), value_weight.astype(bf)], axis=1)
    dvscale = jnp.concatenate([direct_scale, value_scale])[None]
    sbias = jnp.repeat(jnp.transpose(spatial_bias), GDIM, axis=1)
    mg = (merge_weight * merge_scale).astype(bf)
    ex = lax.dynamic_slice_in_dim(expand_weight, r * wide, wide, 1).astype(bf)
    ex = jnp.stack([ex[:, :unit], ex[:, unit:]])
    exscale = lax.dynamic_slice_in_dim(expand_scale, r * wide + f % 2 * unit, unit, 0)[None]
    rd = (lax.dynamic_slice_in_dim(reduce_weight, r * wide, wide, 0) * reduce_scale).astype(bf)
    rd = jnp.transpose(rd.reshape(2, unit, 2, piece // 2), (0, 2, 1, 3))
    seq = 4 * rows
    vm = pltpu.VMEM
    dma = pltpu.SemaphoreType.DMA
    f32 = jnp.float32
    operands = (
        tokens, mixer_gain[None], dv, dvscale, value_gain[None], value_shift[None],
        spatial_weight, sbias, mg, channel_gain[None], ex, exscale, rd,
    )
    return pl.pallas_call(
        fused_kernel,
        out_shape=jax.ShapeDtypeStruct((rows, width), bf),
        in_specs=[pl.BlockSpec(memory_space=pltpu.VMEM)] * len(operands),
        out_specs=pl.BlockSpec(memory_space=pltpu.VMEM),
        scratch_shapes=[
            vm((4, piece, 2 * local), bf),
            vm((4, local, piece), bf),
            vm((4, piece, unit), bf),
            vm((4, 2, unit, piece // 2), bf),
            vm((seq, width), bf),
            vm((seq, 2 * local), f32),
            vm((4, 4, 8, rows), f32),
            vm((seq, local), bf),
            vm((4, seq, piece), bf),
            vm((4, 2 * rows, piece), bf),
            vm((4, rows, piece), bf),
            vm((4, rows, piece), bf),
            vm((rows, width), bf),
            vm((4 * seq, width), bf),
            vm((4 * seq, unit), f32),
            vm((4 * seq, unit), bf),
            vm((8, 4 * seq, piece // 2), bf),
            vm((8, 2 * seq, piece // 2), bf),
            vm((8, seq, piece // 2), bf),
            vm((8, seq, piece // 2), bf),
            vm((8, seq, piece // 2), bf),
            vm((8, 4, rows, piece // 2), bf),
            dma((4,)),
            dma((5, 3)), dma((5, 3)),
            dma((2, 3)), dma((2, 3)),
            dma((3,)), dma((3,)),
            dma((3,)), dma((3,)),
            dma((4, 2)), dma((4, 2)),
            dma((17,)), dma((17,)),
            dma((8, 8)), dma((8, 8)),
        ],
        compiler_params=pltpu.CompilerParams(
            collective_id=0, has_side_effects=True, vmem_limit_bytes=60 * 1024 * 1024
        ),
    )(*operands)


def solution(mesh):
    sizes = mesh.shape
    fused = sizes["rep"] == 2 and sizes["fs"] == 4 and sizes["tp"] == 4
    return jax.shard_map(
        fused_body if fused else body,
        mesh=mesh,
        in_specs=(
            P(("rep", "fs", "tp"), None),
            P(),
            P("fs", "tp"),
            P("tp"),
            P("fs", "tp"),
            P("tp"),
            P("tp"),
            P("tp"),
            P("tp", None, None),
            P("tp", None),
            P("tp", "fs"),
            P("fs"),
            P(),
            P("fs", "tp"),
            P("tp"),
            P("tp", "fs"),
            P("fs"),
        ),
        out_specs=P(("rep", "fs", "tp"), None),
        check_vma=False,
    )
```

```python
import jax
import jax.numpy as jnp
from jax import lax
from jax.experimental import pallas as pl
from jax.experimental.pallas import tpu as pltpu
from jax.sharding import PartitionSpec as P

GDIM = 64
BLOCK = 128


epsilon = 1e-06


def rms_rows(rows, gain):
    floats = rows.astype(jnp.float32)
    scaled = floats * lax.rsqrt(jnp.mean(floats * floats, axis=-1, keepdims=True) + epsilon)
    return (scaled * gain).astype(jnp.bfloat16)


def body(
    tokens,
    mixer_gain,
    direct_weight,
    direct_scale,
    value_weight,
    value_scale,
    value_gain,
    value_shift,
    spatial_weight,
    spatial_bias,
    merge_weight,
    merge_scale,
    channel_gain,
    expand_weight,
    expand_scale,
    reduce_weight,
    reduce_scale,
):
    direct_half = direct_weight.astype(jnp.bfloat16)
    value_half = value_weight.astype(jnp.bfloat16)
    merge_half = merge_weight.astype(jnp.bfloat16)
    expand_half = expand_weight.astype(jnp.bfloat16)
    reduce_half = reduce_weight.astype(jnp.bfloat16)
    full_expand, full_reduce, reduce_full_scale = (
        lax.all_gather(expand_half, "fs", axis=0, tiled=True),
        lax.all_gather(reduce_half, "fs", axis=1, tiled=True),
        lax.all_gather(reduce_scale.astype(jnp.bfloat16), "fs", axis=0, tiled=True).astype(
            reduce_scale.dtype
        ),
    )
    normed = rms_rows(tokens, mixer_gain)
    whole = lax.all_gather(normed, "tp", axis=0, tiled=True)
    seq_rows = whole.shape[0]
    local_width = direct_weight.shape[1]
    direct_pre = jnp.dot(
        whole,
        lax.all_gather(direct_half, "fs", axis=0, tiled=True),
        preferred_element_type=jnp.float32,
    )
    value_pre = jnp.dot(
        whole,
        lax.all_gather(value_half, "fs", axis=0, tiled=True),
        preferred_element_type=jnp.float32,
    )
    full_merge, merge_full_scale = (
        lax.all_gather(merge_half, "fs", axis=1, tiled=True),
        lax.all_gather(merge_scale.astype(jnp.bfloat16), "fs", axis=0, tiled=True).astype(
            merge_scale.dtype
        ),
    )
    direct = jax.nn.gelu(direct_pre * direct_scale)
    value = jax.nn.gelu(value_pre * value_scale)
    total, squares = lax.psum((jnp.sum(value, axis=1), jnp.sum(value * value, axis=1)), "tp")
    branch_width = local_width * lax.axis_size("tp")
    mean = (total / branch_width)[:, None]
    var = (squares / branch_width)[:, None] - mean * mean
    gated_value = ((value - mean) * lax.rsqrt(var + epsilon) * value_gain + value_shift).astype(
        jnp.bfloat16
    )
    local_groups = spatial_weight.shape[0]
    blocks = gated_value.reshape(seq_rows // BLOCK, BLOCK, local_groups, GDIM)
    mixed = jnp.einsum("gpq,nqgc->npgc", spatial_weight, blocks, preferred_element_type=jnp.float32)
    mixed = mixed + jnp.transpose(spatial_bias)[None, :, :, None]
    gated = (direct * mixed.reshape(seq_rows, local_width)).astype(jnp.bfloat16)
    rows = gated
    mix = lax.psum_scatter(
        (jnp.dot(rows, full_merge, preferred_element_type=jnp.float32) * merge_full_scale).astype(
            jnp.bfloat16
        ),
        "tp",
        scatter_dimension=0,
        tiled=True,
    ).astype(jnp.float32)
    middle = (tokens.astype(jnp.float32) + mix).astype(jnp.bfloat16)
    normed_mid = rms_rows(middle, channel_gain)
    whole_mid = lax.all_gather(normed_mid, "tp", axis=0, tiled=True)
    upper = jnp.dot(whole_mid, full_expand, preferred_element_type=jnp.float32)
    hidden = jnp.square(jax.nn.relu(upper * expand_scale)).astype(jnp.bfloat16)
    rows = hidden
    lower = lax.psum_scatter(
        (jnp.dot(rows, full_reduce, preferred_element_type=jnp.float32) * reduce_full_scale).astype(
            jnp.bfloat16
        ),
        "tp",
        scatter_dimension=0,
        tiled=True,
    ).astype(jnp.float32)
    return (middle.astype(jnp.float32) + lower).astype(jnp.bfloat16)


MESH = pl.DeviceIdType.MESH


def fused_kernel(
    tok_ref, mgain_ref, dv_ref, dvscale_ref, vgain_ref, vshift_ref, sw_ref, sbias_ref,
    mg_ref, cgain_ref, ex_ref, exscale_ref, rd_ref,
    out_ref,
    dv_all, mg_all, ex_all, rd_all,
    xg, act, stat, gated, p1, r1, s1, x1, mid,
    nm, acc, hid, p2, r2, s2, z2, s3, x2,
    own_sem, wsend, wrecv, xsend, xrecv, gsend, grecv, tsend, trecv, msend, mrecv, nsend, nrecv, fsend, frecv,
):
    rows, width = tok_ref.shape
    piece = dv_ref.shape[0]
    local = vgain_ref.shape[1]
    seq = xg.shape[0]
    r = lax.axis_index("rep")
    f = lax.axis_index("fs")
    t = lax.axis_index("tp")
    y, c = t // 2, t % 2
    z = f % 2
    mate = f + 1 - 2 * z
    peers = (mate, (f + 2) % 4, (mate + 2) % 4)
    sib = {"tp": y * 2 + (1 - c)}
    ynb = {"tp": (1 - y) * 2 + c}
    xnb = {"rep": 1 - r}
    znb = {"fs": mate}

    barrier = pltpu.get_barrier_semaphore()
    for dev in (sib, ynb, xnb) + tuple({"fs": peer} for peer in peers):
        pl.semaphore_signal(barrier, inc=1, device_id=dev, device_id_type=MESH)
    pl.semaphore_wait(barrier, 6)

    def rcopy(src, dst, ssem, rsem, dev):
        return pltpu.make_async_remote_copy(
            src_ref=src, dst_ref=dst, send_sem=ssem, recv_sem=rsem,
            device_id=dev, device_id_type=MESH,
        )

    mixer = ((dv_ref, dv_all), (mg_ref, mg_all))

    def part(i, slot, q):
        ref = mixer[i][1]
        size = ref.shape[1] // 2
        return ref.at[slot, pl.ds(pl.multiple_of(q * size, size), size)]

    def along(i, j):
        src = mixer[i][0]
        size = src.shape[0] // 2
        return rcopy(
            src.at[pl.ds(pl.multiple_of(r * size, size), size)], part(i, f, r),
            wsend.at[i, j], wrecv.at[i, j], {"fs": peers[j]},
        )

    def over(i, j):
        here = part(i, peers[j], r)
        return rcopy(here, here, xsend.at[i, j], xrecv.at[i, j], xnb)

    def over_start(i):
        for j in range(3):
            along(i, j).wait_recv()
            over(i, j).start()

    def over_wait(i):
        for j in range(3):
            over(i, j).wait_recv()

    def chunk(i, j):
        to = peers[j] % 2
        src = ex_ref.at[to] if i == 2 else rd_ref.at[to, i - 3]
        dst = ex_all.at[f] if i == 2 else rd_all.at[f, i - 3]
        return rcopy(src, dst, wsend.at[i, j], wrecv.at[i, j], {"fs": peers[j]})

    for i in range(2):
        for j in range(3):
            along(i, j).start()
    for j in range(3):
        chunk(2, j).start()
    owns = [
        pltpu.make_async_copy(src, dst.at[f], own_sem.at[i])
        for i, (src, dst) in enumerate(
            mixer + ((ex_ref.at[z], ex_all), (rd_ref.at[z], rd_all))
        )
    ]
    for own in owns:
        own.start()

    def norm(x, gain):
        return (
            x * lax.rsqrt(jnp.mean(x * x, axis=-1, keepdims=True) + epsilon) * gain
        ).astype(jnp.bfloat16)

    def block(n, size=1):
        return pl.ds(pl.multiple_of(n * rows, rows), size * rows)

    def columns(slot):
        return pl.ds(pl.multiple_of(slot * piece, piece), piece)

    mine = xg.at[block(c * 2 + y)]
    mine[...] = norm(tok_ref[...].astype(jnp.float32), mgain_ref[...])
    far = xg.at[block(c * 2 + 1 - y)]
    gather = (
        rcopy(mine, mine, gsend.at[0], grecv.at[0], sib),
        rcopy(mine, mine, gsend.at[1], grecv.at[1], ynb),
        rcopy(far, far, gsend.at[2], grecv.at[2], sib),
    )
    gather[1].start()
    gather[0].start()
    gather[1].wait_recv()
    gather[2].start()
    over_start(0)
    over_start(1)
    gather[0].wait_recv()
    gather[2].wait_recv()
    for own in owns:
        own.wait()

    def project(slot):
        return jnp.dot(xg[:, columns(slot)], dv_all[slot], preferred_element_type=jnp.float32)

    over_wait(0)
    act[...] = project(f)
    for peer in peers:
        act[...] += project(peer)
    act[...] = jax.nn.gelu(act[...] * dvscale_ref[...])

    lane = lax.broadcasted_iota(jnp.int32, (rows, rows), 1)
    for n in range(4):
        value = act[n * rows : (n + 1) * rows, local:]
        total = jnp.sum(value, axis=1, keepdims=True)
        squares = jnp.sum(value * value, axis=1, keepdims=True)
        table = jnp.where(lane == 0, total, jnp.where(lane == 1, squares, 0.0))
        stat[t, n] = jnp.transpose(table)[:8]
    stats = [
        rcopy(stat.at[t], stat.at[t], tsend.at[0], trecv.at[0], sib),
        rcopy(stat.at[t], stat.at[t], tsend.at[1], trecv.at[1], ynb),
        rcopy(
            stat.at[(1 - y) * 2 + c], stat.at[(1 - y) * 2 + c], tsend.at[2], trecv.at[2], sib
        ),
    ]
    stats[1].start()
    stats[0].start()
    stats[1].wait_recv()
    stats[2].start()
    stats[0].wait_recv()
    stats[2].wait_recv()
    inverse = 1.0 / (local * 4)
    group_lane = lax.broadcasted_iota(jnp.int32, (rows, 128), 1) // GDIM
    for n in range(4):
        here = slice(n * rows, (n + 1) * rows)
        summed = stat[0, n] + stat[1, n] + stat[2, n] + stat[3, n]
        table = jnp.transpose(jnp.concatenate([summed] * (rows // 8), axis=0))
        mean = table[:, 0:1] * inverse
        var = table[:, 1:2] * inverse - mean * mean
        gv = (
            (act[here, local:] - mean) * lax.rsqrt(var + epsilon) * vgain_ref[...]
            + vshift_ref[...]
        ).astype(jnp.bfloat16)
        per = 128 // GDIM
        for j in range(local // 128):
            at = slice(j * 128, (j + 1) * 128)
            mixed = jnp.dot(sw_ref[j * per], gv[:, at], preferred_element_type=jnp.float32)
            for k in range(1, per):
                other = jnp.dot(
                    sw_ref[j * per + k], gv[:, at], preferred_element_type=jnp.float32
                )
                mixed = jnp.where(group_lane == k, other, mixed)
            gated[here, at] = (act[here, at] * (mixed + sbias_ref[:, at])).astype(jnp.bfloat16)

    slots = (f,) + peers

    def merge_pair(k):
        return rcopy(
            p1.at[k, block((1 - c) * 2, 2)], r1.at[k], msend.at[k, 0], mrecv.at[k, 0], sib
        )

    def merge_far(k):
        return rcopy(s1.at[k], x1.at[k], msend.at[k, 1], mrecv.at[k, 1], ynb)

    def merge_send(k):
        merge_pair(k).wait_recv()
        s1[k] = (
            p1[k, block(c * 2 + 1 - y)].astype(jnp.float32)
            + r1[k, block(1 - y)].astype(jnp.float32)
        ).astype(jnp.bfloat16)
        merge_far(k).start()

    for k, slot in enumerate(slots):
        if k == 1:
            over_wait(1)
        p1[k] = jnp.dot(gated[...], mg_all[slot], preferred_element_type=jnp.float32).astype(
            jnp.bfloat16
        )
        merge_pair(k).start()
        if k > 0:
            merge_send(k - 1)
    merge_send(3)
    for k, slot in enumerate(slots):
        merge_far(k).wait_recv()
        mid[:, columns(slot)] = (
            tok_ref[:, columns(slot)].astype(jnp.float32)
            + p1[k, block(c * 2 + y)].astype(jnp.float32)
            + r1[k, block(y)].astype(jnp.float32)
            + x1[k].astype(jnp.float32)
        ).astype(jnp.bfloat16)

    def place(zz, rr, yy):
        return nm.at[block(c * 8 + zz * 4 + rr * 2 + yy)]

    half = rows // 2
    mine = place(z, r, y)
    mine[...] = norm(mid[...].astype(jnp.float32), cgain_ref[...])
    over_fs = rcopy(mine, mine, nsend.at[16], nrecv.at[16], znb)

    def spreading(b, zz):
        here = place(zz, r, y)
        from_x, from_y = place(zz, 1 - r, y), place(zz, r, 1 - y)
        from_xy = place(zz, 1 - r, 1 - y)
        low, high = from_x.at[pl.ds(0, half)], from_y.at[pl.ds(half, half)]
        routes = (
            (here, xnb), (here, ynb), (here, sib), (low, ynb), (high, xnb),
            (from_x, sib), (from_y, sib), (from_xy, sib),
        )
        return tuple(
            rcopy(ref, ref, nsend.at[8 * b + k], nrecv.at[8 * b + k], dev)
            for k, (ref, dev) in enumerate(routes)
        )

    near, far = spreading(0, z), spreading(1, 1 - z)
    over_fs.start()
    for i in range(3, 5):
        for j in range(3):
            chunk(i, j).start()
    for k in range(3):
        near[k].start()
    over_fs.wait_recv()
    for k in range(3):
        far[k].start()
    for spread in (near, far):
        for k in range(2):
            spread[k].wait_recv()
            spread[3 + k].start()
            spread[5 + k].start()
    for spread in (near, far):
        spread[3].wait_recv()
        spread[4].wait_recv()
        spread[7].start()
    for spread in (near, far):
        for k in (2, 5, 6, 7):
            spread[k].wait_recv()

    everyone = nm.shape[0]
    tall = 2 * rows

    def over_rows(step):
        lax.fori_loop(
            0, everyone // tall,
            lambda i, _: step(pl.ds(pl.multiple_of(i * tall, tall), tall)), None,
        )

    def expand(at, slot):
        return jnp.dot(nm[at, columns(slot)], ex_all[slot], preferred_element_type=jnp.float32)

    def expand_most(at):
        acc[at] = expand(at, f) + expand(at, peers[0])

    def expand_last(at):
        upper = (acc[at] + expand(at, peers[1]) + expand(at, peers[2])) * exscale_ref[...]
        hid[at] = jnp.square(jax.nn.relu(upper)).astype(jnp.bfloat16)

    chunk(2, 0).wait_recv()
    over_rows(expand_most)
    chunk(2, 1).wait_recv()
    chunk(2, 2).wait_recv()
    over_rows(expand_last)

    def down_pair(k):
        return rcopy(
            p2.at[k, block((1 - c) * 8, 8)], r2.at[k], fsend.at[k, 0], frecv.at[k, 0], sib
        )

    def down_fs(k):
        return rcopy(
            s2.at[k], z2.at[k], fsend.at[k, 7], frecv.at[k, 7], znb
        )

    def down_fs_send(k):
        down_pair(k).wait_recv()
        s2[k] = (
            p2[k, block(c * 8 + (1 - z) * 4, 4)].astype(jnp.float32)
            + r2[k, block((1 - z) * 4, 4)].astype(jnp.float32)
        ).astype(jnp.bfloat16)
        down_fs(k).start()

    hops = ((1 - r, y), (r, 1 - y), (1 - r, 1 - y))

    def down_far(k, h):
        rr, yy = hops[h]
        dev = (xnb, ynb)[h]
        return rcopy(
            s3.at[k, block(rr * 2 + yy)], x2.at[k, h], fsend.at[k, 1 + h], frecv.at[k, 1 + h], dev
        )

    def down_via(k, h):
        return rcopy(
            s3.at[k, pl.ds(pl.multiple_of((hops[2][0] * 2 + hops[2][1]) * rows + h * half, half), half)],
            x2.at[k, 2, pl.ds(h * half, half)],
            fsend.at[k, 3 + h], frecv.at[k, 3 + h], (xnb, ynb)[h],
        )

    def down_on(k, h):
        return rcopy(
            x2.at[k, 2, pl.ds(h * half, half)], x2.at[k, 3, pl.ds(h * half, half)],
            fsend.at[k, 5 + h], frecv.at[k, 5 + h], (ynb, xnb)[h],
        )

    def down_send(k):
        down_fs(k).wait_recv()
        s3[k] = (
            p2[k, block(c * 8 + z * 4, 4)].astype(jnp.float32)
            + r2[k, block(z * 4, 4)].astype(jnp.float32)
            + z2[k].astype(jnp.float32)
        ).astype(jnp.bfloat16)
        for h in range(2):
            down_via(k, h).start()
        for h in range(2):
            down_far(k, h).start()

    def down_relay(k):
        for h in range(2):
            down_via(k, h).wait_recv()
            down_on(k, h).start()

    steps = ((0, 0), (1, 0), (0, 1), (1, 1), (2, 0), (3, 0), (2, 1), (3, 1))
    base = f - z
    order = (base, base + 1, 2 - base, 3 - base)

    def arrived(side, j):
        rcopy(
            rd_ref.at[0, side], rd_all.at[f, side],
            wsend.at[3 + side, j], wrecv.at[3 + side, j], znb,
        ).wait_recv()

    last = len(steps)
    thin = piece // 2

    for k in range(last + 3):
        if k < last:
            from_slot, side = steps[k]
            slot = order[from_slot]
            if from_slot == 0:
                arrived(side, 0)
            elif from_slot > 1:
                arrived(side, 1 + (from_slot + z) % 2)

            def reduce(at, k=k, slot=slot, side=side):
                p2[k, at] = jnp.dot(
                    hid[at], rd_all[slot, side], preferred_element_type=jnp.float32
                ).astype(jnp.bfloat16)

            over_rows(reduce)
            down_pair(k).start()
        if 0 < k <= last:
            down_fs_send(k - 1)
        if 1 < k <= last + 1:
            down_send(k - 2)
        if 2 < k:
            down_relay(k - 3)
    for k, (from_slot, side) in enumerate(steps):
        for h in range(2):
            down_far(k, h).wait_recv()
            down_on(k, h).wait_recv()
        at = pl.ds(pl.multiple_of(order[from_slot] * piece + side * thin, thin), thin)
        out_ref[:, at] = (
            mid[:, at].astype(jnp.float32)
            + p2[k, block(c * 8 + z * 4 + r * 2 + y)].astype(jnp.float32)
            + r2[k, block(z * 4 + r * 2 + y)].astype(jnp.float32)
            + z2[k, block(r * 2 + y)].astype(jnp.float32)
            + x2[k, 0].astype(jnp.float32)
            + x2[k, 1].astype(jnp.float32)
            + x2[k, 3].astype(jnp.float32)
        ).astype(jnp.bfloat16)

    for j in range(3):
        for i in range(2):
            along(i, j).wait_send()
            over(i, j).wait_send()
        for i in range(2, 5):
            chunk(i, j).wait_send()
    for copy in gather + tuple(stats) + near + far + (over_fs,):
        copy.wait_send()
    for k in range(4):
        merge_pair(k).wait_send()
        merge_far(k).wait_send()
    for k in range(last):
        down_pair(k).wait_send()
        down_fs(k).wait_send()
        for h in range(2):
            down_far(k, h).wait_send()
            down_via(k, h).wait_send()
            down_on(k, h).wait_send()


def fused_body(
    tokens,
    mixer_gain,
    direct_weight,
    direct_scale,
    value_weight,
    value_scale,
    value_gain,
    value_shift,
    spatial_weight,
    spatial_bias,
    merge_weight,
    merge_scale,
    channel_gain,
    expand_weight,
    expand_scale,
    reduce_weight,
    reduce_scale,
):
    bf = jnp.bfloat16
    rows, width = tokens.shape
    piece, local = direct_weight.shape
    wide = expand_weight.shape[1] // 2
    r = lax.axis_index("rep")
    unit = wide // 2
    f = lax.axis_index("fs")
    dv = jnp.concatenate([direct_weight.astype(bf), value_weight.astype(bf)], axis=1)
    dvscale = jnp.concatenate([direct_scale, value_scale])[None]
    sbias = jnp.repeat(jnp.transpose(spatial_bias), GDIM, axis=1)
    mg = (merge_weight * merge_scale).astype(bf)
    ex = lax.dynamic_slice_in_dim(expand_weight, r * wide, wide, 1).astype(bf)
    ex = jnp.stack([ex[:, :unit], ex[:, unit:]])
    exscale = lax.dynamic_slice_in_dim(expand_scale, r * wide + f % 2 * unit, unit, 0)[None]
    rd = (lax.dynamic_slice_in_dim(reduce_weight, r * wide, wide, 0) * reduce_scale).astype(bf)
    rd = jnp.transpose(rd.reshape(2, unit, 2, piece // 2), (0, 2, 1, 3))
    seq = 4 * rows
    vm = pltpu.VMEM
    dma = pltpu.SemaphoreType.DMA
    f32 = jnp.float32
    operands = (
        tokens, mixer_gain[None], dv, dvscale, value_gain[None], value_shift[None],
        spatial_weight, sbias, mg, channel_gain[None], ex, exscale, rd,
    )
    return pl.pallas_call(
        fused_kernel,
        out_shape=jax.ShapeDtypeStruct((rows, width), bf),
        in_specs=[pl.BlockSpec(memory_space=pltpu.VMEM)] * len(operands),
        out_specs=pl.BlockSpec(memory_space=pltpu.VMEM),
        scratch_shapes=[
            vm((4, piece, 2 * local), bf),
            vm((4, local, piece), bf),
            vm((4, piece, unit), bf),
            vm((4, 2, unit, piece // 2), bf),
            vm((seq, width), bf),
            vm((seq, 2 * local), f32),
            vm((4, 4, 8, rows), f32),
            vm((seq, local), bf),
            vm((4, seq, piece), bf),
            vm((4, 2 * rows, piece), bf),
            vm((4, rows, piece), bf),
            vm((4, rows, piece), bf),
            vm((rows, width), bf),
            vm((4 * seq, width), bf),
            vm((4 * seq, unit), f32),
            vm((4 * seq, unit), bf),
            vm((8, 4 * seq, piece // 2), bf),
            vm((8, 2 * seq, piece // 2), bf),
            vm((8, seq, piece // 2), bf),
            vm((8, seq, piece // 2), bf),
            vm((8, seq, piece // 2), bf),
            vm((8, 4, rows, piece // 2), bf),
            dma((4,)),
            dma((5, 3)), dma((5, 3)),
            dma((2, 3)), dma((2, 3)),
            dma((3,)), dma((3,)),
            dma((3,)), dma((3,)),
            dma((4, 2)), dma((4, 2)),
            dma((17,)), dma((17,)),
            dma((8, 8)), dma((8, 8)),
        ],
        compiler_params=pltpu.CompilerParams(
            collective_id=0, has_side_effects=True, vmem_limit_bytes=60 * 1024 * 1024
        ),
    )(*operands)


def solution(mesh):
    sizes = mesh.shape
    fused = sizes["rep"] == 2 and sizes["fs"] == 4 and sizes["tp"] == 4
    return jax.shard_map(
        fused_body if fused else body,
        mesh=mesh,
        in_specs=(
            P(("rep", "fs", "tp"), None),
            P(),
            P("fs", "tp"),
            P("tp"),
            P("fs", "tp"),
            P("tp"),
            P("tp"),
            P("tp"),
            P("tp", None, None),
            P("tp", None),
            P("tp", "fs"),
            P("fs"),
            P(),
            P("fs", "tp"),
            P("tp"),
            P("tp", "fs"),
            P("fs"),
        ),
        out_specs=P(("rep", "fs", "tp"), None),
        check_vma=False,
    )
```
